32 devices in a mesh: sp: 4 (over z), fs: 4 (over y, x), tp: 2 (over core).
Axes of the slice: x: 2, y: 2, z: 4, core: 2. Of those that a mesh axis runs over, the one named last changes fastest.
Arguments:
- tokens: bfloat16 [4096, 2048], P(('fs', 'sp', 'tp')), parts along dimension 0, may hold values from -6 to 6
- norm_gain: float32 [2048], replicated, may hold values from 0.1 to 1.9
- recurrent_input: bfloat16 [2048, 1024], P(None, 'tp'), may hold values from -0.125 to 0.125
- recurrent_gate: bfloat16 [2048, 1024], P(None, 'tp'), may hold values from -0.125 to 0.125
- attention_gate: bfloat16 [2048, 1024], P(None, 'tp'), may hold values from -0.125 to 0.125
- query_proj: bfloat16 [2048, 1536], P(None, 'tp'), may hold values from -0.125 to 0.125
- latent_down: bfloat16 [2048, 512], P(None, 'tp'), may hold values from -0.125 to 0.125
- rope_key_down: bfloat16 [2048, 64], replicated, may hold values from -0.125 to 0.125
- conv_kernel: float32 [4, 1024], P(None, 'tp'), may hold values from -3 to 3
- recurrence_gate_blocks: bfloat16 [16, 64, 64], P('tp'), may hold values from -0.75 to 0.75
- input_gate_blocks: bfloat16 [16, 64, 64], P('tp'), may hold values from -0.75 to 0.75
- decay_rate: float32 [1024], P('tp'), as said below
- decay_shift: float32 [4096], P(('fs', 'sp')), parts along dimension 0, may hold values from -2 to 0, as said below
- initial_state: float32 [4096], P(('fs', 'tp')), parts along dimension 0, may hold values from -6 to 6
- latent_gain: float32 [512], replicated, may hold values from 0.1 to 1.9
- latent_up: bfloat16 [512, 2048], P(None, 'tp'), may hold values from -0.25 to 0.25
- query_gain: float32 [192], replicated, may hold values from 0.4 to 250, as said below
- recurrent_output: bfloat16 [1024, 2048], P('tp'), may hold values from -0.25 to 0.25
- attention_output: bfloat16 [1024, 2048], P('tp'), may hold values from -0.25 to 0.25
Outputs:
- mixed_output: bfloat16 [4096, 2048], P(('fs', 'sp', 'tp')), parts along dimension 0
The draws below stay inside these ranges and needn't reach their ends.
There are 4 independent parts, one for each index of `fs`. The reference program is written for one: setup_inputs(seed, part) draws one part's arguments, and reference() takes and returns one part's arrays. A program takes and returns all parts, laid end to end along the dimension named above; an argument that names none is the same for every part. Nothing has to cross between parts.
Inputs may be any that keep to these rules, and one draw needn't show every extreme that they name: `decay_rate`: positive. `decay_shift`: negative. `query_gain`: positive.
All inputs are finite; a program needn't handle non-finite values.
Results may differ from the reference program's by a relative error of at most 0.03.
The reference program's roundings to bfloat16 on the way count: a program that leaves them out, or rounds other values in their place, can miss the bound.
Values may be sent and summed in bfloat16 or wider, within the bound.
A program may use at most 128 MiB of HBM per device.

```python
import math
import jax
import jax.numpy as jnp
from jax import lax

D = 2048
DR = 1024
BLK = 64
BLOCKS = 16
CONV = 4
H = 8
NOPE = 128
ROPE = 64
VH = 128
LAT = 512
DA = 1024
TOK_DEV = 256
SEQUENCE_LENGTH = 1024
N_TP = 2


def draw_decay_rate(key, part):
    pick_key, slow_key, fast_key = jax.random.split(key, 3)
    slow_share = 0.5
    slow_mask = jax.random.bernoulli(pick_key, slow_share, (DR,))
    slow_rate = jnp.exp(jax.random.uniform(slow_key, (DR,), jnp.float32, jnp.log(0.05), jnp.log(1.0))) / (8.0 * SEQUENCE_LENGTH)
    fast_rate = jnp.exp(jax.random.uniform(fast_key, (DR,), jnp.float32, jnp.log(0.004), jnp.log(0.012)))
    return jnp.where(slow_mask, slow_rate, fast_rate)


def draw_decay_shift(key, part):
    level_key, place_key, depth_key = jax.random.split(key, 3)
    block_count = SEQUENCE_LENGTH // TOK_DEV
    levels = jnp.exp(jax.random.uniform(level_key, (block_count,), jnp.float32, jnp.log(0.05), jnp.log(0.5))) / SEQUENCE_LENGTH
    baseline_offset = -jnp.repeat(levels, TOK_DEV)
    slot_indices = jax.random.randint(place_key, (2,), 0, SEQUENCE_LENGTH)
    layer_depths = jnp.log(jax.random.uniform(depth_key, (2,), jnp.float32, 0.5, 0.8))
    spike_flags = jnp.arange(SEQUENCE_LENGTH)[:, None] == slot_indices[None, :]
    return baseline_offset + jnp.sum(jnp.where(spike_flags, layer_depths[None, :], 0.0), axis=1)


def draw_query_gain(key, part):
    gain_key = jax.random.fold_in(key, 0)
    gain_values = jax.random.uniform(gain_key, (NOPE + ROPE,), jnp.float32, 0.4, 1.6)
    return gain_values


def level_of(rng, extent, cuts, least, high):
    level = 1.0
    for axis_at, parts in cuts:
        heights = jax.random.uniform(jax.random.fold_in(jax.random.fold_in(rng, 6), axis_at), (parts,), jnp.float32, least / len(cuts), high / len(cuts))
        level = level * jnp.repeat(jnp.exp(heights), extent[axis_at] // parts).reshape((-1,) + (1,) * (len(extent) - 1 - axis_at))
    return level


def scatter_about(key, extent, scale, bound, cuts=(), kind=jnp.bfloat16):
    array = scale * jax.random.normal(key, extent, jnp.float32)
    if cuts:
        array = array * level_of(key, extent, cuts, -0.22, 0.18)
    return jnp.clip(array, -bound, bound).astype(kind)


def setup_inputs(seed: int = 0, part: int = 0) -> dict:
    splits = jax.random.split(jax.random.key(seed), 20)
    part_keys = jax.random.split(jax.random.fold_in(splits[19], part), 20)
    return {
        "tokens": scatter_about(part_keys[0], (SEQUENCE_LENGTH, D), 1.0, 6.0, ((0, 8),)),
        "norm_gain": jnp.clip(1.0 + 0.18 * jax.random.normal(splits[1], (D,), jnp.float32), 0.1, 1.9),
        "recurrent_input": scatter_about(splits[2], (D, DR), D ** -0.5, 0.125, ((1, 2),)),
        "recurrent_gate": scatter_about(splits[3], (D, DR), D ** -0.5, 0.125, ((1, 2),)),
        "attention_gate": scatter_about(splits[4], (D, DA), D ** -0.5, 0.125, ((1, 2),)),
        "query_proj": scatter_about(splits[5], (D, H * (NOPE + ROPE)), D ** -0.5, 0.125, ((1, 2),)),
        "latent_down": scatter_about(splits[6], (D, LAT), D ** -0.5, 0.125, ((1, 2),)),
        "rope_key_down": scatter_about(splits[7], (D, ROPE), D ** -0.5, 0.125),
        "conv_kernel": scatter_about(splits[8], (CONV, DR), 0.5, 3.0, ((1, 2),), jnp.float32),
        "recurrence_gate_blocks": scatter_about(splits[9], (BLOCKS, BLK, BLK), BLK ** -0.5, 0.75, ((0, 2),)),
        "input_gate_blocks": scatter_about(splits[10], (BLOCKS, BLK, BLK), BLK ** -0.5, 0.75, ((0, 2),)),
        "decay_rate": draw_decay_rate(jax.random.fold_in(splits[19], 71), part),
        "decay_shift": draw_decay_shift(jax.random.fold_in(jax.random.fold_in(splits[19], part), 71), part),
        "initial_state": scatter_about(part_keys[13], (DR,), 1.0, 6.0, ((0, 2),), jnp.float32),
        "latent_gain": jnp.clip(1.0 + 0.18 * jax.random.normal(splits[14], (LAT,), jnp.float32), 0.1, 1.9),
        "latent_up": scatter_about(splits[15], (LAT, H * (NOPE + VH)), LAT ** -0.5, 0.25, ((1, 2),)),
        "query_gain": draw_query_gain(jax.random.fold_in(splits[19], 71), part),
        "recurrent_output": scatter_about(splits[17], (DR, D), ((DR + DA) // 4) ** -0.5, 0.25, ((0, 2),)),
        "attention_output": scatter_about(splits[18], (DA, D), ((DR + DA) // 4) ** -0.5, 0.25, ((0, 2),)),
    }


EPS = 1e-06
RECURRENT_SCALE = 8.0
THETA = 10000.0

def rotate_half(values, token_positions):
    half_width = values.shape[-1] // 2
    inv_freq = 1.0 / THETA ** (jnp.arange(0, 2 * half_width, 2, dtype=jnp.float32) / (2 * half_width))
    angles = token_positions.astype(jnp.float32)[:, None] * inv_freq[None, :]
    cosine = jnp.cos(angles)
    sine_part = jnp.sin(angles)
    if values.ndim == 3:
        cosine = cosine[:, None, :]
        sine_part = sine_part[:, None, :]
    first_half = values[..., :half_width]
    second_half = values[..., half_width:]
    return jnp.concatenate([first_half * cosine - second_half * sine_part, first_half * sine_part + second_half * cosine], axis=-1)

def rms_scaled(values, gain_vec):
    return values * lax.rsqrt(lax.optimization_barrier(jnp.mean(values * values, axis=-1, keepdims=True)) + EPS) * gain_vec

def rounded(values):
    return lax.optimization_barrier(values.astype(jnp.bfloat16)).astype(jnp.float32)

def linear_step(earlier, later_part):
    return (earlier[0] * later_part[0], later_part[0] * earlier[1] + later_part[1])

def reference(tokens, norm_gain, recurrent_input, recurrent_gate, attention_gate, query_proj, latent_down, rope_key_down, conv_kernel, recurrence_gate_blocks, input_gate_blocks, decay_rate, decay_shift, initial_state, latent_gain, latent_up, query_gain, recurrent_output, attention_output):
    normed = rms_scaled(tokens.astype(jnp.float32), norm_gain).astype(jnp.bfloat16)

    def project(weight):
        return jnp.dot(normed, weight, preferred_element_type=jnp.float32).astype(jnp.bfloat16)
    recur_signal = project(recurrent_input)
    recur_gate_pre = project(recurrent_gate)
    attention_pre = project(attention_gate)
    query_raw = project(query_proj)
    latent_raw = project(latent_down)
    rope_raw = project(rope_key_down)
    token_positions = jnp.arange(SEQUENCE_LENGTH, dtype=jnp.int32)
    padded = jnp.concatenate([jnp.zeros((CONV - 1, DR), jnp.bfloat16), recur_signal], axis=0).astype(jnp.float32)
    conv_sum = conv_kernel[0] * padded[0:SEQUENCE_LENGTH]
    for tap_index in range(1, CONV):
        conv_sum = conv_sum + conv_kernel[tap_index] * padded[tap_index:tap_index + SEQUENCE_LENGTH]
    conv_back = rounded(conv_sum)
    grouped = conv_back.reshape(SEQUENCE_LENGTH, BLOCKS, BLK)
    recur_rate = jax.nn.sigmoid(jnp.einsum('tbi,bij->tbj', grouped, recurrence_gate_blocks.astype(jnp.float32)).reshape(SEQUENCE_LENGTH, DR))
    input_rate = jax.nn.sigmoid(jnp.einsum('tbi,bij->tbj', grouped, input_gate_blocks.astype(jnp.float32)).reshape(SEQUENCE_LENGTH, DR))
    log_decay = -RECURRENT_SCALE * recur_rate * decay_rate + decay_shift[:, None]
    decay = jnp.exp(log_decay)
    driven = jnp.sqrt(-jnp.expm1(2.0 * log_decay)) * input_rate * conv_back
    driven = driven.at[0].add(decay[0] * initial_state)
    decay_prod, states = lax.associative_scan(linear_step, (decay, driven), axis=0)
    recur_out = (states * jax.nn.silu(recur_gate_pre.astype(jnp.float32))).astype(jnp.bfloat16)
    query_rows = rms_scaled(query_raw.astype(jnp.float32).reshape(SEQUENCE_LENGTH, H, NOPE + ROPE), query_gain)
    query_rows = jnp.concatenate([query_rows[..., :NOPE], rotate_half(query_rows[..., NOPE:], token_positions)], axis=-1).astype(jnp.bfloat16)
    latent = rms_scaled(latent_raw.astype(jnp.float32), latent_gain).astype(jnp.bfloat16)
    key_values = jnp.dot(latent, latent_up, preferred_element_type=jnp.float32).astype(jnp.bfloat16).reshape(SEQUENCE_LENGTH, H, NOPE + VH)
    key_nope = key_values[..., :NOPE].astype(jnp.float32)
    values_all = key_values[..., NOPE:].astype(jnp.float32)
    key_rope = rotate_half(rope_raw.astype(jnp.float32), token_positions).astype(jnp.bfloat16).astype(jnp.float32)
    query_block = math.gcd(SEQUENCE_LENGTH, 512)
    score_scale = (NOPE + ROPE) ** (-0.5)

    def attend(block_index):
        begin_row = (block_index * query_block).astype(jnp.int32)
        query_part = lax.dynamic_slice_in_dim(query_rows, begin_row, query_block, 0).astype(jnp.float32)
        scores = jnp.einsum('thd,khd->htk', query_part[..., :NOPE], key_nope)
        scores = scores + jnp.einsum('thr,kr->htk', query_part[..., NOPE:], key_rope)
        scores = scores * score_scale
        query_pos = begin_row + jnp.arange(query_block, dtype=jnp.int32)
        allowed = token_positions[None, None, :] <= query_pos[None, :, None]
        scores = jnp.where(allowed, scores, -jnp.inf)
        row_max = lax.optimization_barrier(jnp.max(scores, axis=-1, keepdims=True))
        weights = jnp.exp(scores - row_max)
        denominator = lax.optimization_barrier(jnp.sum(weights, axis=-1))
        weighted = jnp.einsum('htk,khd->thd', rounded(weights), values_all)
        return weighted / jnp.transpose(denominator)[:, :, None]
    attended = lax.map(attend, jnp.arange(SEQUENCE_LENGTH // query_block, dtype=jnp.int32)).reshape(SEQUENCE_LENGTH, DA)
    attention_out = (attended * jax.nn.silu(attention_pre.astype(jnp.float32))).astype(jnp.bfloat16)
    recur_group = DR // N_TP
    attend_group = DA // N_TP

    def add_group(group_index, running):
        index_value = group_index.astype(jnp.int32)
        recur_part = lax.dynamic_slice_in_dim(recur_out, index_value * recur_group, recur_group, 1)
        recur_rows = lax.dynamic_slice_in_dim(recurrent_output, index_value * recur_group, recur_group, 0)
        attend_part = lax.dynamic_slice_in_dim(attention_out, index_value * attend_group, attend_group, 1)
        attend_rows = lax.dynamic_slice_in_dim(attention_output, index_value * attend_group, attend_group, 0)
        partial_sum = jnp.dot(recur_part, recur_rows, preferred_element_type=jnp.float32) + jnp.dot(attend_part, attend_rows, preferred_element_type=jnp.float32)
        return running + rounded(partial_sum)
    total = lax.fori_loop(0, N_TP, add_group, jnp.zeros((SEQUENCE_LENGTH, D), jnp.float32))
    return total.astype(jnp.bfloat16)
```

```python
import math

import jax
import jax.numpy as jnp
from jax import lax
from jax.experimental import pallas as pl
from jax.experimental.pallas import tpu as pltpu
from jax.sharding import PartitionSpec as P

EPS = 1e-06
RECURRENT_SCALE = 8.0
THETA = 10000.0


def from_behind(block, axis, distance):
    devices = range(lax.axis_size(axis))
    route = [(i - distance, i) for i in devices if i - distance in devices]
    return lax.ppermute(block, axis, route)


def expm1_neg(y):
    small = y * (1.0 + y * (0.5 + y * (1.0 / 6 + y * (1.0 / 24 + y * (1.0 / 120 + y / 720)))))
    return jnp.where(y > -0.35, small, jnp.exp(y) - 1.0)


def block_diagonal(scratch, blocks_ref, first):
    size = blocks_ref.shape[1]
    scratch[...] = jnp.zeros_like(scratch)
    for k in range(scratch.shape[0] // size):
        scratch[k * size : (k + 1) * size, k * size : (k + 1) * size] = blocks_ref[first + k]
    return scratch[...]


def scan_rows(decay, state):
    rows = decay.shape[0]
    row = lax.broadcasted_iota(jnp.int32, decay.shape, 0)
    step = 1
    while step < rows:
        inside = row >= step
        before_decay = jnp.where(inside, pltpu.roll(decay, step, 0), 1.0)
        before_state = jnp.where(inside, pltpu.roll(state, step, 0), 0.0)
        state = state + decay * before_state
        decay = decay * before_decay
        step *= 2
    return decay, state


def recurrence_kernel(
    rim_ref, signal_ref, kernel_ref, rec_ref, inp_ref, rate_ref, shift_ref,
    prod_ref, state_ref, ext, diag_a, diag_b,
):
    rows, width = signal_ref.shape
    taps = kernel_ref.shape[0]
    lanes = diag_a.shape[0]
    ext[0:8] = rim_ref[...].astype(jnp.float32)
    ext[8 : 8 + rows] = signal_ref[...].astype(jnp.float32)
    size = rec_ref.shape[1]
    for c in range(width // lanes):
        cols = slice(c * lanes, (c + 1) * lanes)
        conv = kernel_ref[0:1, cols] * ext[9 - taps : 9 - taps + rows, cols]
        for j in range(1, taps):
            conv = conv + kernel_ref[j : j + 1, cols] * ext[9 - taps + j : 9 - taps + j + rows, cols]
        conv = conv.astype(jnp.bfloat16)
        per = lanes // size
        rec = jax.nn.sigmoid(
            jnp.dot(conv, block_diagonal(diag_a, rec_ref, c * per), preferred_element_type=jnp.float32)
        )
        inp = jax.nn.sigmoid(
            jnp.dot(conv, block_diagonal(diag_b, inp_ref, c * per), preferred_element_type=jnp.float32)
        )
        log_decay = -RECURRENT_SCALE * rec * rate_ref[0:1, cols] + shift_ref[...]
        driven = jnp.sqrt(-expm1_neg(2.0 * log_decay)) * inp * conv.astype(jnp.float32)
        prod, state = scan_rows(jnp.exp(log_decay), driven)
        prod_ref[:, cols] = prod
        state_ref[:, cols] = state


def rotate_half(values, token_positions):
    half_width = values.shape[-1] // 2
    inv_freq = 1.0 / THETA ** (
        jnp.arange(0, 2 * half_width, 2, dtype=jnp.float32) / (2 * half_width)
    )
    angles = token_positions.astype(jnp.float32)[:, None] * inv_freq[None, :]
    cosine = jnp.cos(angles)
    sine_part = jnp.sin(angles)
    if values.ndim == 3:
        cosine = cosine[:, None, :]
        sine_part = sine_part[:, None, :]
    first_half = values[..., :half_width]
    second_half = values[..., half_width:]
    return jnp.concatenate(
        [
            first_half * cosine - second_half * sine_part,
            first_half * sine_part + second_half * cosine,
        ],
        axis=-1,
    )


def rms_scaled(values, gain_vec):
    return values * lax.rsqrt(jnp.mean(values * values, axis=-1, keepdims=True) + EPS) * gain_vec


def body(
    tokens,
    norm_gain,
    recurrent_input,
    recurrent_gate,
    attention_gate,
    query_proj,
    latent_down,
    rope_key_down,
    conv_kernel,
    recurrence_gate_blocks,
    input_gate_blocks,
    decay_rate,
    decay_shift,
    initial_state,
    latent_gain,
    latent_up,
    query_gain,
    recurrent_output,
    attention_output,
):
    tp_count = lax.axis_size("tp")
    sp_count = lax.axis_size("sp")
    sp_place = lax.axis_index("sp")
    tp_place = lax.axis_index("tp")
    channel_width = recurrent_input.shape[1]
    value_width = attention_gate.shape[1]
    query_width = query_proj.shape[1]
    latent_width = latent_down.shape[1]
    rope_width = rope_key_down.shape[1]
    head_dim = query_gain.shape[0]
    nope_width = head_dim - rope_width
    local_heads = query_width // head_dim
    head_value = value_width // local_heads
    normed = rms_scaled(
        lax.all_gather(tokens, "tp", axis=0, tiled=True).astype(jnp.float32), norm_gain
    ).astype(jnp.bfloat16)
    recur_signal, recur_gate_pre, attention_pre, query_raw, latent_local, rope_raw = [
        jnp.dot(normed, weight, preferred_element_type=jnp.float32).astype(jnp.bfloat16)
        for weight in (
            recurrent_input, recurrent_gate, attention_gate, query_proj, latent_down, rope_key_down,
        )
    ]
    local_tokens = normed.shape[0]
    token_positions = sp_place * local_tokens + jnp.arange(local_tokens, dtype=jnp.int32)
    taps = conv_kernel.shape[0]
    conv_rim = from_behind(recur_signal[local_tokens - taps + 1 :], "sp", 1)
    rim8 = jnp.pad(conv_rim, ((8 - taps + 1, 0), (0, 0)))
    lanes = min(128, channel_width)
    shape = jax.ShapeDtypeStruct((local_tokens, channel_width), jnp.float32)
    decay_prod, zero_state = pl.pallas_call(
        recurrence_kernel,
        out_shape=(shape, shape),
        scratch_shapes=[
            pltpu.VMEM((local_tokens + 8, channel_width), jnp.float32),
            pltpu.VMEM((lanes, lanes), jnp.bfloat16),
            pltpu.VMEM((lanes, lanes), jnp.bfloat16),
        ],
    )(
        rim8, recur_signal, conv_kernel, recurrence_gate_blocks, input_gate_blocks,
        decay_rate[None], decay_shift[:, None],
    )
    parts = lax.all_gather(jnp.stack([decay_prod[-1], zero_state[-1]]), "sp")
    incoming = initial_state
    for hop in range(sp_count - 1):
        use = hop < sp_place
        incoming = jnp.where(use, parts[hop, 0] * incoming + parts[hop, 1], incoming)
    states = zero_state + decay_prod * incoming
    recur_out = (states * jax.nn.silu(recur_gate_pre.astype(jnp.float32))).astype(jnp.bfloat16)
    query_rows = rms_scaled(
        query_raw.astype(jnp.float32).reshape(local_tokens, local_heads, head_dim), query_gain
    )
    query_rows = jnp.concatenate(
        [query_rows[..., :nope_width], rotate_half(query_rows[..., nope_width:], token_positions)],
        axis=-1,
    ).astype(jnp.bfloat16)
    query_nope = query_rows[..., :nope_width]
    query_rope = query_rows[..., nope_width:]
    rope_share = rope_width // tp_count
    rotary_portion = lax.dynamic_slice_in_dim(rope_raw, tp_place * rope_share, rope_share, 1)
    outgoing = jnp.concatenate([latent_local, rotary_portion], axis=1)
    arrived = lax.all_gather(outgoing, ("sp", "tp"), axis=1, tiled=True)
    grid_view = arrived.reshape(local_tokens, sp_count, tp_count, latent_width + rope_share)
    key_count = local_tokens * sp_count
    latent_all = grid_view[..., :latent_width].reshape(key_count, tp_count * latent_width)
    rope_all = grid_view[..., latent_width:].reshape(key_count, rope_width)
    key_positions = (
        jnp.arange(sp_count, dtype=jnp.int32)[None, :] * local_tokens
        + jnp.arange(local_tokens, dtype=jnp.int32)[:, None]
    ).reshape(key_count)
    normed_latent = rms_scaled(latent_all.astype(jnp.float32), latent_gain).astype(jnp.bfloat16)
    expanded = jnp.dot(normed_latent, latent_up, preferred_element_type=jnp.float32).astype(
        jnp.bfloat16
    )
    key_rope = rotate_half(rope_all.astype(jnp.float32), key_positions).astype(jnp.bfloat16)
    head_keys = expanded.reshape(key_count, local_heads, nope_width + head_value)
    key_nope = head_keys[..., :nope_width]
    key_values = head_keys[..., nope_width:]
    key_group = math.gcd(sp_count, 4)
    block_keys = local_tokens * key_group
    block_total = key_count // block_keys
    score_scale = head_dim ** (-0.5)

    def online_step(block_index, carried):
        running_max, total_weight, weighted = carried
        begin_key = block_index * block_keys
        nope_block = lax.dynamic_slice_in_dim(key_nope, begin_key, block_keys, 0)
        rope_block = lax.dynamic_slice_in_dim(key_rope, begin_key, block_keys, 0)
        pos_block = lax.dynamic_slice_in_dim(key_positions, begin_key, block_keys, 0)
        value_block = lax.dynamic_slice_in_dim(key_values, begin_key, block_keys, 0)
        scores = jnp.einsum(
            "thd,khd->htk", query_nope, nope_block, preferred_element_type=jnp.float32
        )
        scores = scores + jnp.einsum(
            "thr,kr->htk", query_rope, rope_block, preferred_element_type=jnp.float32
        )
        scores = scores * score_scale
        allowed = pos_block[None, :] <= token_positions[:, None]
        scores = jnp.where(allowed[None], scores, -jnp.inf)
        new_max = jnp.maximum(running_max, jnp.max(scores, axis=-1))
        rescale = jnp.exp(running_max - new_max)
        weights = jnp.exp(scores - new_max[..., None])
        block_weighted = jnp.einsum(
            "htk,khd->thd",
            weights.astype(jnp.bfloat16),
            value_block,
            preferred_element_type=jnp.float32,
        )
        weighted = weighted * jnp.transpose(rescale)[:, :, None] + block_weighted
        total_weight = total_weight * rescale + jnp.sum(weights, axis=-1)
        return (new_max, total_weight, weighted)

    start_sums = (
        jnp.full((local_heads, local_tokens), -jnp.inf, jnp.float32),
        jnp.zeros((local_heads, local_tokens), jnp.float32),
        jnp.zeros((local_tokens, local_heads, head_value), jnp.float32),
    )
    row_max, total_weight, weighted = lax.fori_loop(0, block_total, online_step, start_sums)
    attended = weighted / jnp.transpose(total_weight)[:, :, None]
    attention_out = (
        attended.reshape(local_tokens, value_width) * jax.nn.silu(attention_pre.astype(jnp.float32))
    ).astype(jnp.bfloat16)
    return lax.psum_scatter(
        (
            jnp.dot(recur_out, recurrent_output, preferred_element_type=jnp.float32)
            + jnp.dot(attention_out, attention_output, preferred_element_type=jnp.float32)
        ).astype(jnp.bfloat16),
        "tp",
        scatter_dimension=0,
        tiled=True,
    )


def solution(mesh):
    return jax.shard_map(
        body,
        mesh=mesh,
        in_specs=(
            P(("fs", "sp", "tp"), None),
            P(),
            P(None, "tp"),
            P(None, "tp"),
            P(None, "tp"),
            P(None, "tp"),
            P(None, "tp"),
            P(),
            P(None, "tp"),
            P("tp", None, None),
            P("tp", None, None),
            P("tp"),
            P(("fs", "sp")),
            P(("fs", "tp")),
            P(),
            P(None, "tp"),
            P(),
            P("tp", None),
            P("tp", None),
        ),
        out_specs=P(("fs", "sp", "tp"), None),
        check_vma=False,
    )
```

```python
import functools

import jax
import jax.numpy as jnp
import numpy as np
from jax import lax
from jax.experimental import pallas as pl
from jax.experimental.pallas import tpu as pltpu
from jax.sharding import PartitionSpec as P

EPS = 1e-06
RECURRENT_SCALE = 8.0
THETA = 10000.0
F32 = jnp.float32
BF16 = jnp.bfloat16
LANES = 128


def expm1_neg(y):
    small = y * (1.0 + y * (0.5 + y * (1.0 / 6 + y * (1.0 / 24 + y * (1.0 / 120 + y / 720)))))
    return jnp.where(y > -0.35, small, jnp.exp(y) - 1.0)


def block_diagonal(scratch, blocks_ref, first):
    size = blocks_ref.shape[1]
    scratch[...] = jnp.zeros_like(scratch)
    for k in range(scratch.shape[0] // size):
        scratch[k * size : (k + 1) * size, k * size : (k + 1) * size] = blocks_ref[first + k]
    return scratch[...]


def scan_rows(decay, state):
    rows = decay.shape[0]
    row = lax.broadcasted_iota(jnp.int32, decay.shape, 0)
    step = 1
    while step < rows:
        inside = row >= step
        before_decay = jnp.where(inside, pltpu.roll(decay, step, 0), 1.0)
        before_state = jnp.where(inside, pltpu.roll(state, step, 0), 0.0)
        state = state + decay * before_state
        decay = decay * before_decay
        step *= 2
    return decay, state


def rms_scaled(values, gain_vec):
    return values * lax.rsqrt(jnp.mean(values * values, axis=-1, keepdims=True) + EPS) * gain_vec


def rotary_tables(positions, width):
    half = width // 2
    inv_freq = (1.0 / THETA ** (np.arange(0, width, 2, dtype=np.float32) / width)).astype(np.float32)
    angles = np.arange(positions, dtype=np.float32)[:, None] * inv_freq[None, :]
    cosine = np.cos(angles.astype(np.float64)).astype(np.float32)
    sine = np.sin(angles.astype(np.float64)).astype(np.float32)
    return np.concatenate([cosine, cosine], 1), np.concatenate([-sine, sine], 1)


def rotate(values, cosine, sine):
    half = values.shape[-1] // 2
    swapped = jnp.concatenate([values[:, half:], values[:, :half]], axis=1)
    return values * cosine + swapped * sine


def column_step(width):
    return 256 if width % 256 == 0 else width


def remote(src, dst, send, recv, **where):
    return pltpu.make_async_remote_copy(
        src_ref=src, dst_ref=dst, send_sem=send, recv_sem=recv,
        device_id=where, device_id_type=pl.DeviceIdType.MESH,
    )


def layer_kernel(
    sp_count, tp_count,
    tokens, norm_gain, conv_kernel, rec_blocks, inp_blocks, decay_rate, decay_shift,
    initial_state, latent_gain, query_gain, cos_table, sin_table,
    h_lat, h_rope, h_in, h_gate, h_query, h_att, h_up, h_rout, h_aout,
    out,
    w_lat, w_rope, w_in, w_gate, w_query, w_att, w_up, w_rout, w_aout,
    tok_all, normed, lat_all, sig, gate, attp, qraw, rim_in, ext, diag_a, diag_b,
    prod, state, car_out, car_in, rout, racc, queries, kv, row_max, row_sum, acc, aout,
    part, part_in,
    w_sem, tok_s, tok_r, z_s, z_r, l_s, l_r, rim_s, rim_r, c_s, c_r, p_s, p_r,
):
    sp = lax.axis_index("sp")
    tp = lax.axis_index("tp")
    group = sp_count * tp_count
    share = tokens.shape[0]
    rows = normed.shape[0]
    taps, width = conv_kernel.shape
    head_dim = query_gain.shape[1]
    rope = w_rope.shape[1]
    nope = head_dim - rope
    heads = w_query.shape[1] // head_dim
    lat = w_lat.shape[1]
    value = attp.shape[1] // heads

    pairs = list(zip(
        (h_lat, h_rope, h_in, h_query, h_gate, h_att, h_up, h_rout, h_aout),
        (w_lat, w_rope, w_in, w_query, w_gate, w_att, w_up, w_rout, w_aout),
    ))
    loads = [pltpu.make_async_copy(a, b, w_sem.at[k]) for k, (a, b) in enumerate(pairs)]
    for load in loads:
        load.start()
    l_lat, l_rope, l_in, l_query, l_gate, l_att, l_up, l_rout, l_aout = loads

    barrier = pltpu.get_barrier_semaphore()

    def greet(d, carry):
        other = lax.rem(sp * tp_count + tp + d, group)
        pl.semaphore_signal(
            barrier, inc=1,
            device_id={"sp": other // tp_count, "tp": lax.rem(other, tp_count)},
            device_id_type=pl.DeviceIdType.MESH,
        )
        return carry

    lax.fori_loop(1, group, greet, 0)
    pl.semaphore_wait(barrier, group - 1)

    def peer(d):
        return lax.rem(tp + d, tp_count)

    def source(d):
        return lax.rem(tp - d + tp_count, tp_count)

    def token_copy(d):
        return remote(tokens, tok_all.at[d - 1], tok_s.at[d - 1], tok_r.at[d - 1], tp=peer(d))

    for d in range(1, tp_count):
        token_copy(d).start()

    def put_normed(block, place):
        normed[pl.ds(pl.multiple_of(place * share, share), share)] = rms_scaled(
            block.astype(F32), norm_gain[...]
        ).astype(BF16)

    put_normed(tokens[...], tp)
    for d in range(1, tp_count):
        token_copy(d).wait_recv()
        put_normed(tok_all[d - 1], source(d))

    def project(weight, into):
        step = column_step(weight.shape[1])
        for c in range(weight.shape[1] // step):
            cols = slice(c * step, (c + 1) * step)
            into[:, cols] = jnp.dot(
                normed[...], weight[:, cols], preferred_element_type=F32
            ).astype(BF16)

    l_lat.wait()
    l_rope.wait()
    own = lat_all.at[sp, tp]
    own[:, :lat] = jnp.dot(normed[...], w_lat[...], preferred_element_type=F32).astype(BF16)
    own[:, lat:] = jnp.dot(normed[...], w_rope[...], preferred_element_type=F32).astype(BF16)

    def along(e):
        block = lat_all.at[sp, tp]
        return remote(block, block, z_s.at[e - 1], z_r.at[e - 1], sp=sp + e)

    def landed(e):
        block = lat_all.at[sp - e, tp]
        return remote(block, block, z_s.at[e - 1], z_r.at[e - 1], sp=sp - e)

    def across(e, d):
        block = lat_all.at[sp - e, tp]
        return remote(block, block, l_s.at[e, d - 1], l_r.at[e, d - 1], tp=peer(d))

    def crossed(e, d):
        block = lat_all.at[sp - e, source(d)]
        return remote(block, block, l_s.at[e, d - 1], l_r.at[e, d - 1], tp=source(d))

    for e in range(1, sp_count):
        pl.when(sp + e < sp_count)(lambda e=e: along(e).start())
    for d in range(1, tp_count):
        across(0, d).start()

    l_in.wait()
    project(w_in, sig)

    def rim_copy():
        return remote(sig.at[pl.ds(rows - 16, 16)], rim_in, rim_s, rim_r, sp=sp + 1)

    def rim_landed():
        return remote(sig.at[pl.ds(rows - 16, 16)], rim_in, rim_s, rim_r, sp=sp - 1)

    pl.when(sp + 1 < sp_count)(lambda: rim_copy().start())

    @pl.when(sp == 0)
    def _():
        rim_in[...] = jnp.zeros_like(rim_in)

    l_query.wait()
    project(w_query, qraw)
    here = pl.ds(pl.multiple_of(sp * rows, rows), rows)
    for h in range(heads):
        head = rms_scaled(qraw[:, h * head_dim : (h + 1) * head_dim].astype(F32), query_gain[...])
        turned = rotate(head[:, nope:], cos_table[here], sin_table[here])
        queries[h, :, :nope] = head[:, :nope].astype(BF16)
        queries[h, :, nope:] = turned.astype(BF16)

    pl.when(sp > 0)(lambda: rim_landed().wait_recv())
    ext[0:8] = rim_in[8:16].astype(F32)
    ext[8 : 8 + rows] = sig[...].astype(F32)
    size = rec_blocks.shape[1]
    car_out[...] = jnp.zeros_like(car_out)
    shift = jnp.broadcast_to(decay_shift[...], (LANES, rows)).T
    for c in range(width // LANES):
        cols = slice(c * LANES, (c + 1) * LANES)
        conv = conv_kernel[0:1, cols] * ext[9 - taps : 9 - taps + rows, cols]
        for j in range(1, taps):
            first = 9 - taps + j
            conv = conv + conv_kernel[j : j + 1, cols] * ext[first : first + rows, cols]
        conv = conv.astype(BF16)
        per = LANES // size
        rec = jax.nn.sigmoid(
            jnp.dot(conv, block_diagonal(diag_a, rec_blocks, c * per), preferred_element_type=F32)
        )
        inp = jax.nn.sigmoid(
            jnp.dot(conv, block_diagonal(diag_b, inp_blocks, c * per), preferred_element_type=F32)
        )
        log_decay = -RECURRENT_SCALE * rec * decay_rate[0:1, cols] + shift
        driven = jnp.sqrt(-expm1_neg(2.0 * log_decay)) * inp * conv.astype(F32)
        one, two = scan_rows(jnp.exp(log_decay), driven)
        prod[:, cols] = one
        state[:, cols] = two
        car_out[0:1, cols] = one[rows - 1 :]
        car_out[1:2, cols] = two[rows - 1 :]

    def carry_copy(e):
        return remote(car_out, car_in.at[e - 1], c_s.at[e - 1], c_r.at[e - 1], sp=sp + e)

    def carry_landed(e):
        return remote(car_out, car_in.at[e - 1], c_s.at[e - 1], c_r.at[e - 1], sp=sp - e)

    for e in range(1, sp_count):
        pl.when(sp + e < sp_count)(lambda e=e: carry_copy(e).start())

    l_gate.wait()
    project(w_gate, gate)
    l_att.wait()
    project(w_att, attp)
    l_up.wait()

    for e in range(1, sp_count):

        @pl.when(sp >= e)
        def _(e=e):
            landed(e).wait_recv()
            for d in range(1, tp_count):
                across(e, d).start()

    scale = head_dim ** (-0.5)

    def attend(e, diagonal):
        place = sp - e
        blocks = [lat_all[place, n, :, :lat].astype(F32) for n in range(tp_count)]
        square = sum(jnp.sum(x * x, axis=-1, keepdims=True) for x in blocks)
        inverse = lax.rsqrt(square / (lat * tp_count) + EPS)
        total = None
        for n, x in enumerate(blocks):
            x = (x * inverse * latent_gain[0:1, n * lat : (n + 1) * lat]).astype(BF16)
            term = jnp.dot(x, w_up[n * lat : (n + 1) * lat], preferred_element_type=F32)
            total = term if total is None else total + term
        kv[...] = total.astype(BF16)
        there = pl.ds(pl.multiple_of(place * rows, rows), rows)
        turned = rotate(
            lat_all[place, tp, :, lat:].astype(F32), cos_table[there], sin_table[there]
        ).astype(BF16)
        for h in range(heads):
            base = h * (nope + value)
            keys = jnp.concatenate([kv[:, base : base + nope], turned], axis=1)
            scores = lax.dot_general(
                queries[h], keys, (((1,), (1,)), ((), ())), preferred_element_type=F32
            ) * scale
            if diagonal:
                seen = lax.broadcasted_iota(jnp.int32, scores.shape, 1)
                scores = jnp.where(
                    seen <= lax.broadcasted_iota(jnp.int32, scores.shape, 0), scores, -jnp.inf
                )
            top = jnp.max(scores, axis=-1, keepdims=True)
            if not diagonal:
                before = row_max[h, :, 0:1]
                top = jnp.maximum(top, before)
                fade = jnp.exp(before - top)
            weights = jnp.exp(scores - top)
            mass = jnp.sum(weights, axis=-1, keepdims=True)
            term = jnp.dot(
                weights.astype(BF16), kv[:, base + nope : base + nope + value],
                preferred_element_type=F32,
            )
            if not diagonal:
                mass = mass + row_sum[h, :, 0:1] * fade
                term = term + acc[h] * fade
            row_max[h] = jnp.broadcast_to(top, (rows, LANES))
            row_sum[h] = jnp.broadcast_to(mass, (rows, LANES))
            acc[h] = term

    for d in range(1, tp_count):
        crossed(0, d).wait_recv()
    attend(0, True)

    for e in range(1, sp_count):

        @pl.when(sp >= e)
        def _(e=e):
            carry_landed(e).wait_recv()

        @pl.when(sp < e)
        def _(e=e):
            car_in[e - 1, 0:1] = jnp.ones((1, width), F32)
            car_in[e - 1, 1:2] = jnp.zeros((1, width), F32)

    incoming = initial_state[...]
    for e in range(sp_count - 1, 0, -1):
        incoming = car_in[e - 1, 0:1] * incoming + car_in[e - 1, 1:2]
    for c in range(width // LANES):
        cols = slice(c * LANES, (c + 1) * LANES)
        full = state[:, cols] + prod[:, cols] * incoming[:, cols]
        rout[:, cols] = (full * jax.nn.silu(gate[:, cols].astype(F32))).astype(BF16)
    l_rout.wait()
    model = out.shape[1]
    step = column_step(model)
    for c in range(model // step):
        cols = slice(c * step, (c + 1) * step)
        racc[:, cols] = jnp.dot(rout[...], w_rout[:, cols], preferred_element_type=F32)

    def earlier(e, carry):
        for d in range(1, tp_count):
            crossed(e, d).wait_recv()
        attend(e, False)
        return carry

    lax.fori_loop(1, sp + 1, earlier, 0)
    for h in range(heads):
        cols = slice(h * value, (h + 1) * value)
        aout[:, cols] = (
            acc[h] / row_sum[h, :, 0:1] * jax.nn.silu(attp[:, cols].astype(F32))
        ).astype(BF16)
    l_aout.wait()
    for c in range(model // step):
        cols = slice(c * step, (c + 1) * step)
        both = racc[:, cols] + jnp.dot(aout[...], w_aout[:, cols], preferred_element_type=F32)
        part[:, :, cols] = both.astype(BF16).reshape(tp_count, share, step)

    def part_copy(d):
        return remote(part.at[peer(d)], part_in.at[d - 1], p_s.at[d - 1], p_r.at[d - 1], tp=peer(d))

    for d in range(1, tp_count):
        part_copy(d).start()
    for d in range(1, tp_count):
        part_copy(d).wait_recv()
    summed = part[tp].astype(F32)
    for d in range(1, tp_count):
        summed = summed + part_in[d - 1].astype(F32)
    out[...] = summed.astype(BF16)

    for d in range(1, tp_count):
        token_copy(d).wait_send()
        across(0, d).wait_send()
        part_copy(d).wait_send()
    pl.when(sp + 1 < sp_count)(lambda: rim_copy().wait_send())
    for e in range(1, sp_count):

        @pl.when(sp + e < sp_count)
        def _(e=e):
            along(e).wait_send()
            carry_copy(e).wait_send()

        @pl.when(sp >= e)
        def _(e=e):
            for d in range(1, tp_count):
                across(e, d).wait_send()


def body(
    tokens, norm_gain, recurrent_input, recurrent_gate, attention_gate, query_proj, latent_down,
    rope_key_down, conv_kernel, recurrence_gate_blocks, input_gate_blocks, decay_rate, decay_shift,
    initial_state, latent_gain, latent_up, query_gain, recurrent_output, attention_output,
):
    tp_count = lax.axis_size("tp")
    sp_count = lax.axis_size("sp")
    share, model = tokens.shape
    rows = share * tp_count
    width = recurrent_input.shape[1]
    taken = attention_gate.shape[1]
    head_dim = query_gain.shape[0]
    heads = query_proj.shape[1] // head_dim
    value = taken // heads
    lat = latent_down.shape[1]
    rope = rope_key_down.shape[1]
    cos_table, sin_table = rotary_tables(sp_count * rows, rope)
    hbm = [
        latent_down, rope_key_down, recurrent_input, recurrent_gate, query_proj, attention_gate,
        latent_up, recurrent_output, attention_output,
    ]
    small = [
        tokens, norm_gain[None], conv_kernel, recurrence_gate_blocks, input_gate_blocks,
        decay_rate[None], decay_shift[None], initial_state[None], latent_gain[None],
        query_gain[None], jnp.asarray(cos_table), jnp.asarray(sin_table),
    ]
    vmem = pltpu.VMEM
    dma = pltpu.SemaphoreType.DMA
    others = max(tp_count - 1, 1)
    hops = max(sp_count - 1, 1)
    return pl.pallas_call(
        functools.partial(layer_kernel, sp_count, tp_count),
        out_shape=jax.ShapeDtypeStruct((share, model), BF16),
        in_specs=[pl.BlockSpec(memory_space=pltpu.VMEM)] * len(small)
        + [pl.BlockSpec(memory_space=pl.ANY)] * len(hbm),
        out_specs=pl.BlockSpec(memory_space=pltpu.VMEM),
        scratch_shapes=[vmem(a.shape, a.dtype) for a in hbm]
        + [
            vmem((others, share, model), BF16),
            vmem((rows, model), BF16),
            vmem((sp_count, tp_count, rows, lat + rope), BF16),
            vmem((rows, width), BF16),
            vmem((rows, width), BF16),
            vmem((rows, taken), BF16),
            vmem((rows, query_proj.shape[1]), BF16),
            vmem((16, width), BF16),
            vmem((rows + 8, width), F32),
            vmem((LANES, LANES), BF16),
            vmem((LANES, LANES), BF16),
            vmem((rows, width), F32),
            vmem((rows, width), F32),
            vmem((8, width), F32),
            vmem((hops, 8, width), F32),
            vmem((rows, width), BF16),
            vmem((rows, model), F32),
            vmem((heads, rows, head_dim), BF16),
            vmem((rows, latent_up.shape[1]), BF16),
            vmem((heads, rows, LANES), F32),
            vmem((heads, rows, LANES), F32),
            vmem((heads, rows, value), F32),
            vmem((rows, taken), BF16),
            vmem((tp_count, share, model), BF16),
            vmem((others, share, model), BF16),
            dma((len(hbm),)),
            dma((others,)), dma((others,)),
            dma((hops,)), dma((hops,)),
            dma((sp_count, others)), dma((sp_count, others)),
            dma, dma,
            dma((hops,)), dma((hops,)),
            dma((others,)), dma((others,)),
        ],
        compiler_params=pltpu.CompilerParams(
            collective_id=0, has_side_effects=True, vmem_limit_bytes=60 * 1024 * 1024
        ),
    )(*small, *hbm)


def solution(mesh):
    return jax.shard_map(
        body,
        mesh=mesh,
        in_specs=(
            P(("fs", "sp", "tp"), None),
            P(),
            P(None, "tp"),
            P(None, "tp"),
            P(None, "tp"),
            P(None, "tp"),
            P(None, "tp"),
            P(),
            P(None, "tp"),
            P("tp", None, None),
            P("tp", None, None),
            P("tp"),
            P(("fs", "sp")),
            P(("fs", "tp")),
            P(),
            P(None, "tp"),
            P(),
            P("tp", None),
            P("tp", None),
        ),
        out_specs=P(("fs", "sp", "tp"), None),
        check_vma=False,
    )
```

```python
import functools

import jax
import jax.numpy as jnp
import numpy as np
from jax import lax
from jax.experimental import pallas as pl
from jax.experimental.pallas import tpu as pltpu
from jax.sharding import PartitionSpec as P

EPS = 1e-06
RECURRENT_SCALE = 8.0
THETA = 10000.0
F32 = jnp.float32
BF16 = jnp.bfloat16
LANES = 128


def expm1_neg(y):
    small = y * (1.0 + y * (0.5 + y * (1.0 / 6 + y * (1.0 / 24 + y * (1.0 / 120 + y / 720)))))
    return jnp.where(y > -0.35, small, jnp.exp(y) - 1.0)


def block_diagonal(scratch, blocks_ref, first):
    size = blocks_ref.shape[1]
    scratch[...] = jnp.zeros_like(scratch)
    for k in range(scratch.shape[0] // size):
        scratch[k * size : (k + 1) * size, k * size : (k + 1) * size] = blocks_ref[first + k]
    return scratch[...]


def scan_rows(decay, state):
    rows = decay.shape[0]
    row = lax.broadcasted_iota(jnp.int32, decay.shape, 0)
    step = 1
    while step < rows:
        inside = row >= step
        before_decay = jnp.where(inside, pltpu.roll(decay, step, 0), 1.0)
        before_state = jnp.where(inside, pltpu.roll(state, step, 0), 0.0)
        state = state + decay * before_state
        decay = decay * before_decay
        step *= 2
    return decay, state


def rms_scaled(values, gain_vec):
    return values * lax.rsqrt(jnp.mean(values * values, axis=-1, keepdims=True) + EPS) * gain_vec


def rotary_tables(positions, width):
    half = width // 2
    inv_freq = (1.0 / THETA ** (np.arange(0, width, 2, dtype=np.float32) / width)).astype(np.float32)
    angles = np.arange(positions, dtype=np.float32)[:, None] * inv_freq[None, :]
    cosine = np.cos(angles.astype(np.float64)).astype(np.float32)
    sine = np.sin(angles.astype(np.float64)).astype(np.float32)
    return np.concatenate([cosine, cosine], 1), np.concatenate([-sine, sine], 1)


def rotate(values, cosine, sine):
    half = values.shape[-1] // 2
    swapped = jnp.concatenate([values[:, half:], values[:, :half]], axis=1)
    return values * cosine + swapped * sine


def column_step(width):
    return 256 if width % 256 == 0 else width


def remote(src, dst, send, recv, **where):
    return pltpu.make_async_remote_copy(
        src_ref=src, dst_ref=dst, send_sem=send, recv_sem=recv,
        device_id=where, device_id_type=pl.DeviceIdType.MESH,
    )


def layer_kernel(
    sp_count, tp_count,
    tokens, norm_gain, conv_kernel, rec_blocks, inp_blocks, decay_rate, decay_shift,
    initial_state, latent_gain, query_gain, cos_table, sin_table,
    h_lat, h_rope, h_in, h_gate, h_query, h_att, h_up, h_rout, h_aout,
    out,
    w_lat, w_rope, w_in, w_gate, w_query, w_att, w_up, w_rout, w_aout,
    tok_all, normed, lat_all, sig, gate, attp, qraw, rim_in, ext, diag_a, diag_b,
    prod, state, car_out, car_in, rout, racc, queries, kv, row_max, row_sum, acc, aout,
    part, part_in,
    w_sem, tok_s, tok_r, z_s, z_r, l_s, l_r, rim_s, rim_r, c_s, c_r, p_s, p_r,
):
    sp = lax.axis_index("sp")
    tp = lax.axis_index("tp")
    group = sp_count * tp_count
    share = tokens.shape[0]
    rows = normed.shape[0]
    taps, width = conv_kernel.shape
    head_dim = query_gain.shape[1]
    rope = w_rope.shape[0]
    nope = head_dim - rope
    heads = w_query.shape[1] // head_dim
    lat = w_lat.shape[1]
    value = attp.shape[1] // heads
    packed = lat // rope
    tall = share // packed

    pairs = list(zip(
        (h_in, h_lat, h_rope, h_query, h_gate, h_att, h_up, h_rout, h_aout),
        (w_in, w_lat, w_rope, w_query, w_gate, w_att, w_up, w_rout, w_aout),
    ))
    loads = [pltpu.make_async_copy(a, b, w_sem.at[k]) for k, (a, b) in enumerate(pairs)]
    for load in loads:
        load.start()
    l_in, l_lat, l_rope, l_query, l_gate, l_att, l_up, l_rout, l_aout = loads

    barrier = pltpu.get_barrier_semaphore()

    def greet(d, carry):
        other = lax.rem(sp * tp_count + tp + d, group)
        pl.semaphore_signal(
            barrier, inc=1,
            device_id={"sp": other // tp_count, "tp": lax.rem(other, tp_count)},
            device_id_type=pl.DeviceIdType.MESH,
        )
        return carry

    lax.fori_loop(1, group, greet, 0)
    pl.semaphore_wait(barrier, group - 1)

    def peer(d):
        return lax.rem(tp + d, tp_count)

    def source(d):
        return lax.rem(tp - d + tp_count, tp_count)

    def token_copy(d):
        return remote(tokens, tok_all.at[d - 1], tok_s.at[d - 1], tok_r.at[d - 1], tp=peer(d))

    for d in range(1, tp_count):
        token_copy(d).start()

    def put_normed(block, place):
        normed[pl.ds(pl.multiple_of(place * share, share), share)] = rms_scaled(
            block.astype(F32), norm_gain[...]
        ).astype(BF16)

    put_normed(tokens[...], tp)
    for d in range(1, tp_count):
        token_copy(d).wait_recv()
        put_normed(tok_all[d - 1], source(d))

    def project(weight, into):
        step = column_step(weight.shape[1])
        for c in range(weight.shape[1] // step):
            cols = slice(c * step, (c + 1) * step)
            into[:, cols] = jnp.dot(
                normed[...], weight[:, cols], preferred_element_type=F32
            ).astype(BF16)

    l_in.wait()
    project(w_in, sig)

    def rim_copy():
        return remote(sig.at[pl.ds(rows - 16, 16)], rim_in, rim_s, rim_r, sp=sp + 1)

    def rim_landed():
        return remote(sig.at[pl.ds(rows - 16, 16)], rim_in, rim_s, rim_r, sp=sp - 1)

    pl.when(sp + 1 < sp_count)(lambda: rim_copy().start())

    @pl.when(sp == 0)
    def _():
        rim_in[...] = jnp.zeros_like(rim_in)

    l_lat.wait()
    l_rope.wait()
    own = lat_all.at[sp, tp]
    own[:rows] = jnp.dot(normed[...], w_lat[...], preferred_element_type=F32).astype(BF16)
    mine = normed[pl.ds(pl.multiple_of(tp * share, share), share)]
    keyed = lax.dot_general(
        mine, w_rope[...], (((1,), (1,)), ((), ())), preferred_element_type=F32
    )
    for k in range(packed):
        own[rows:, k * rope : (k + 1) * rope] = keyed[k * tall : (k + 1) * tall].astype(BF16)

    def along(e):
        block = lat_all.at[sp - e, tp]
        return remote(block, block, z_s.at[e], z_r.at[e], sp=sp + 1)

    def landed(e):
        block = lat_all.at[sp - e, tp]
        return remote(block, block, z_s.at[e - 1], z_r.at[e - 1], sp=sp - 1)

    def across(e, d):
        block = lat_all.at[sp - e, tp]
        return remote(block, block, l_s.at[e, d - 1], l_r.at[e, d - 1], tp=peer(d))

    def crossed(e, d):
        block = lat_all.at[sp - e, source(d)]
        return remote(block, block, l_s.at[e, d - 1], l_r.at[e, d - 1], tp=source(d))

    if sp_count > 1:
        pl.when(sp + 1 < sp_count)(lambda: along(0).start())
    for d in range(1, tp_count):
        across(0, d).start()

    def relay(e):
        @pl.when(sp >= e)
        def _():
            landed(e).wait_recv()
            if e + 1 < sp_count:
                pl.when(sp + 1 < sp_count)(lambda: along(e).start())
            for d in range(1, tp_count):
                across(e, d).start()

    l_query.wait()
    project(w_query, qraw)
    here = pl.ds(pl.multiple_of(sp * rows, rows), rows)
    for h in range(heads):
        head = rms_scaled(qraw[:, h * head_dim : (h + 1) * head_dim].astype(F32), query_gain[...])
        turned = rotate(head[:, nope:], cos_table[here], sin_table[here])
        queries[h, :, :nope] = head[:, :nope].astype(BF16)
        queries[h, :, nope:] = turned.astype(BF16)

    for e in range(1, min(2, sp_count)):
        relay(e)
    pl.when(sp > 0)(lambda: rim_landed().wait_recv())
    ext[0:8] = rim_in[8:16].astype(F32)
    ext[8 : 8 + rows] = sig[...].astype(F32)
    size = rec_blocks.shape[1]
    car_out[...] = jnp.zeros_like(car_out)
    shift = jnp.broadcast_to(decay_shift[...], (LANES, rows)).T
    for c in range(width // LANES):
        cols = slice(c * LANES, (c + 1) * LANES)
        conv = conv_kernel[0:1, cols] * ext[9 - taps : 9 - taps + rows, cols]
        for j in range(1, taps):
            first = 9 - taps + j
            conv = conv + conv_kernel[j : j + 1, cols] * ext[first : first + rows, cols]
        conv = conv.astype(BF16)
        per = LANES // size
        rec = jax.nn.sigmoid(
            jnp.dot(conv, block_diagonal(diag_a, rec_blocks, c * per), preferred_element_type=F32)
        )
        inp = jax.nn.sigmoid(
            jnp.dot(conv, block_diagonal(diag_b, inp_blocks, c * per), preferred_element_type=F32)
        )
        log_decay = -RECURRENT_SCALE * rec * decay_rate[0:1, cols] + shift
        driven = jnp.sqrt(-expm1_neg(2.0 * log_decay)) * inp * conv.astype(F32)
        one, two = scan_rows(jnp.exp(log_decay), driven)
        prod[:, cols] = one
        state[:, cols] = two
        car_out[0:1, cols] = one[rows - 1 :]
        car_out[1:2, cols] = two[rows - 1 :]

    def carry_copy(e):
        return remote(car_out, car_in.at[e - 1], c_s.at[e - 1], c_r.at[e - 1], sp=sp + e)

    def carry_landed(e):
        return remote(car_out, car_in.at[e - 1], c_s.at[e - 1], c_r.at[e - 1], sp=sp - e)

    for e in range(1, sp_count):
        pl.when(sp + e < sp_count)(lambda e=e: carry_copy(e).start())

    for e in range(2, min(3, sp_count)):
        relay(e)
    l_gate.wait()
    project(w_gate, gate)
    l_att.wait()
    project(w_att, attp)
    l_up.wait()

    for e in range(3, sp_count):
        relay(e)

    scale = head_dim ** (-0.5)

    def attend(e, diagonal):
        place = sp - e
        blocks = [lat_all[place, n, :rows].astype(F32) for n in range(tp_count)]
        square = sum(jnp.sum(x * x, axis=-1, keepdims=True) for x in blocks)
        inverse = lax.rsqrt(square / (lat * tp_count) + EPS)
        total = None
        for n, x in enumerate(blocks):
            x = (x * inverse * latent_gain[0:1, n * lat : (n + 1) * lat]).astype(BF16)
            term = jnp.dot(x, w_up[n * lat : (n + 1) * lat], preferred_element_type=F32)
            total = term if total is None else total + term
        kv[...] = total.astype(BF16)
        there = pl.ds(pl.multiple_of(place * rows, rows), rows)
        raw = jnp.concatenate(
            [
                lat_all[place, n, rows:, k * rope : (k + 1) * rope].astype(F32)
                for n in range(tp_count)
                for k in range(packed)
            ],
            axis=0,
        )
        turned = rotate(raw, cos_table[there], sin_table[there]).astype(BF16)
        for h in range(heads):
            base = h * (nope + value)
            keys = jnp.concatenate([kv[:, base : base + nope], turned], axis=1)
            scores = lax.dot_general(
                queries[h], keys, (((1,), (1,)), ((), ())), preferred_element_type=F32
            ) * scale
            if diagonal:
                seen = lax.broadcasted_iota(jnp.int32, scores.shape, 1)
                scores = jnp.where(
                    seen <= lax.broadcasted_iota(jnp.int32, scores.shape, 0), scores, -jnp.inf
                )
            top = jnp.max(scores, axis=-1, keepdims=True)
            if not diagonal:
                before = row_max[h, :, 0:1]
                top = jnp.maximum(top, before)
                fade = jnp.exp(before - top)
            weights = jnp.exp(scores - top)
            mass = jnp.sum(weights, axis=-1, keepdims=True)
            term = jnp.dot(
                weights.astype(BF16), kv[:, base + nope : base + nope + value],
                preferred_element_type=F32,
            )
            if not diagonal:
                mass = mass + row_sum[h, :, 0:1] * fade
                term = term + acc[h] * fade
            row_max[h] = jnp.broadcast_to(top, (rows, LANES))
            row_sum[h] = jnp.broadcast_to(mass, (rows, LANES))
            acc[h] = term

    for d in range(1, tp_count):
        crossed(0, d).wait_recv()
    attend(0, True)

    for e in range(1, sp_count):

        @pl.when(sp >= e)
        def _(e=e):
            carry_landed(e).wait_recv()

        @pl.when(sp < e)
        def _(e=e):
            car_in[e - 1, 0:1] = jnp.ones((1, width), F32)
            car_in[e - 1, 1:2] = jnp.zeros((1, width), F32)

    incoming = initial_state[...]
    for e in range(sp_count - 1, 0, -1):
        incoming = car_in[e - 1, 0:1] * incoming + car_in[e - 1, 1:2]
    for c in range(width // LANES):
        cols = slice(c * LANES, (c + 1) * LANES)
        full = state[:, cols] + prod[:, cols] * incoming[:, cols]
        rout[:, cols] = (full * jax.nn.silu(gate[:, cols].astype(F32))).astype(BF16)
    l_rout.wait()
    model = out.shape[1]
    step = column_step(model)
    for c in range(model // step):
        cols = slice(c * step, (c + 1) * step)
        racc[:, cols] = jnp.dot(rout[...], w_rout[:, cols], preferred_element_type=F32)

    def earlier(e, carry):
        for d in range(1, tp_count):
            crossed(e, d).wait_recv()
        attend(e, False)
        return carry

    lax.fori_loop(1, sp + 1, earlier, 0)
    for h in range(heads):
        cols = slice(h * value, (h + 1) * value)
        aout[:, cols] = (
            acc[h] / row_sum[h, :, 0:1] * jax.nn.silu(attp[:, cols].astype(F32))
        ).astype(BF16)
    l_aout.wait()
    for c in range(model // step):
        cols = slice(c * step, (c + 1) * step)
        both = racc[:, cols] + jnp.dot(aout[...], w_aout[:, cols], preferred_element_type=F32)
        part[:, :, cols] = both.astype(BF16).reshape(tp_count, share, step)

    def part_copy(d):
        return remote(part.at[peer(d)], part_in.at[d - 1], p_s.at[d - 1], p_r.at[d - 1], tp=peer(d))

    for d in range(1, tp_count):
        part_copy(d).start()
    for d in range(1, tp_count):
        part_copy(d).wait_recv()
    summed = part[tp].astype(F32)
    for d in range(1, tp_count):
        summed = summed + part_in[d - 1].astype(F32)
    out[...] = summed.astype(BF16)

    for d in range(1, tp_count):
        token_copy(d).wait_send()
        across(0, d).wait_send()
        part_copy(d).wait_send()
    pl.when(sp + 1 < sp_count)(lambda: rim_copy().wait_send())
    for e in range(1, sp_count):

        @pl.when(sp + e < sp_count)
        def _(e=e):
            carry_copy(e).wait_send()

        @pl.when((sp >= e - 1) & (sp + 1 < sp_count))
        def _(e=e):
            along(e - 1).wait_send()

        @pl.when(sp >= e)
        def _(e=e):
            for d in range(1, tp_count):
                across(e, d).wait_send()


def body(
    tokens, norm_gain, recurrent_input, recurrent_gate, attention_gate, query_proj, latent_down,
    rope_key_down, conv_kernel, recurrence_gate_blocks, input_gate_blocks, decay_rate, decay_shift,
    initial_state, latent_gain, latent_up, query_gain, recurrent_output, attention_output,
):
    tp_count = lax.axis_size("tp")
    sp_count = lax.axis_size("sp")
    share, model = tokens.shape
    rows = share * tp_count
    width = recurrent_input.shape[1]
    taken = attention_gate.shape[1]
    head_dim = query_gain.shape[0]
    heads = query_proj.shape[1] // head_dim
    value = taken // heads
    lat = latent_down.shape[1]
    rope = rope_key_down.shape[1]
    cos_table, sin_table = rotary_tables(sp_count * rows, rope)
    hbm = [
        latent_down, rope_key_down.T, recurrent_input, recurrent_gate, query_proj, attention_gate,
        latent_up, recurrent_output, attention_output,
    ]
    small = [
        tokens, norm_gain[None], conv_kernel, recurrence_gate_blocks, input_gate_blocks,
        decay_rate[None], decay_shift[None], initial_state[None], latent_gain[None],
        query_gain[None], jnp.asarray(cos_table), jnp.asarray(sin_table),
    ]
    vmem = pltpu.VMEM
    dma = pltpu.SemaphoreType.DMA
    others = max(tp_count - 1, 1)
    hops = max(sp_count - 1, 1)
    return pl.pallas_call(
        functools.partial(layer_kernel, sp_count, tp_count),
        out_shape=jax.ShapeDtypeStruct((share, model), BF16),
        in_specs=[pl.BlockSpec(memory_space=pltpu.VMEM)] * len(small)
        + [pl.BlockSpec(memory_space=pl.ANY)] * len(hbm),
        out_specs=pl.BlockSpec(memory_space=pltpu.VMEM),
        scratch_shapes=[vmem(a.shape, a.dtype) for a in hbm]
        + [
            vmem((others, share, model), BF16),
            vmem((rows, model), BF16),
            vmem((sp_count, tp_count, rows + share * rope // lat, lat), BF16),
            vmem((rows, width), BF16),
            vmem((rows, width), BF16),
            vmem((rows, taken), BF16),
            vmem((rows, query_proj.shape[1]), BF16),
            vmem((16, width), BF16),
            vmem((rows + 8, width), F32),
            vmem((LANES, LANES), BF16),
            vmem((LANES, LANES), BF16),
            vmem((rows, width), F32),
            vmem((rows, width), F32),
            vmem((8, width), F32),
            vmem((hops, 8, width), F32),
            vmem((rows, width), BF16),
            vmem((rows, model), F32),
            vmem((heads, rows, head_dim), BF16),
            vmem((rows, latent_up.shape[1]), BF16),
            vmem((heads, rows, LANES), F32),
            vmem((heads, rows, LANES), F32),
            vmem((heads, rows, value), F32),
            vmem((rows, taken), BF16),
            vmem((tp_count, share, model), BF16),
            vmem((others, share, model), BF16),
            dma((len(hbm),)),
            dma((others,)), dma((others,)),
            dma((hops,)), dma((hops,)),
            dma((sp_count, others)), dma((sp_count, others)),
            dma, dma,
            dma((hops,)), dma((hops,)),
            dma((others,)), dma((others,)),
        ],
        compiler_params=pltpu.CompilerParams(
            collective_id=0, has_side_effects=True, vmem_limit_bytes=60 * 1024 * 1024
        ),
    )(*small, *hbm)


def solution(mesh):
    return jax.shard_map(
        body,
        mesh=mesh,
        in_specs=(
            P(("fs", "sp", "tp"), None),
            P(),
            P(None, "tp"),
            P(None, "tp"),
            P(None, "tp"),
            P(None, "tp"),
            P(None, "tp"),
            P(),
            P(None, "tp"),
            P("tp", None, None),
            P("tp", None, None),
            P("tp"),
            P(("fs", "sp")),
            P(("fs", "tp")),
            P(),
            P(None, "tp"),
            P(),
            P("tp", None),
            P("tp", None),
        ),
        out_specs=P(("fs", "sp", "tp"), None),
        check_vma=False,
    )
```
